32 devices in a mesh: ep: 4 (over y, x), tp: 8 (over z, core).
Axes of the slice: x: 2, y: 2, z: 4, core: 2. Of those that a mesh axis runs over, the one named last changes fastest.
Arguments:
- resid: bfloat16 [512, 2048], P('ep'), may hold values from -6 to 6
- norm1_gain: float32 [2048], replicated, may hold values from 0.1 to 1.9
- w_query: bfloat16 [2048, 2048], P('ep', 'tp'), may hold values from -0.125 to 0.125
- w_key: bfloat16 [2048, 2048], P('ep', 'tp'), may hold values from -0.125 to 0.125
- w_value: bfloat16 [2048, 2048], P('ep', 'tp'), may hold values from -0.125 to 0.125
- w_outgate: bfloat16 [2048, 2048], P('ep', 'tp'), may hold values from -0.125 to 0.125
- w_igate: bfloat16 [2048, 32], replicated, may hold values from -0.125 to 0.125
- w_fgate: bfloat16 [2048, 32], replicated, may hold values from -0.125 to 0.125
- forget_bias: float32 [32], replicated, may hold values from 0 to 4
- head_gain: float32 [2048], P('tp'), may hold values from 0.1 to 1.9
- w_out: bfloat16 [2048, 2048], P('tp'), may hold values from -0.125 to 0.125
- state_matrix: float32 [512, 32, 64, 64], P('ep', 'tp'), may hold values from -4 to 4
- state_norm: float32 [512, 32, 64], P('ep', 'tp'), may hold values from -8 to 8
- state_max: float32 [512, 32], P('ep', 'tp'), may hold values from -1 to 2
- norm2_gain: float32 [2048], replicated, may hold values from 0.1 to 1.9
- group_router: bfloat16 [2048, 4], replicated, may hold values from -0.125 to 0.125
- expert_router: bfloat16 [2048, 8], replicated, may hold values from -0.125 to 0.125
- expert_ids: int32 [512, 2], P('ep'), may hold values from 0 to 7, all different within a row; in each aligned block of 128 rows (0 to 127, 128 to 255, ...) at most 48 rows name the same one
- exp_gate: bfloat16 [8, 2048, 1024], P('ep', None, 'tp'), may hold values from -0.125 to 0.125
- exp_up: bfloat16 [8, 2048, 1024], P('ep', None, 'tp'), may hold values from -0.125 to 0.125
- exp_down: bfloat16 [8, 1024, 2048], P('ep', 'tp'), may hold values from -0.1875 to 0.1875
Outputs:
- mixed: bfloat16 [512, 2048], P('ep', 'tp')
- new_matrix: float32 [512, 32, 64, 64], P('ep', 'tp')
- new_normer: float32 [512, 32, 64], P('ep', 'tp')
- new_max: float32 [512, 32], P('ep', 'tp')
The draws below stay inside these ranges and needn't reach their ends.
Inputs may be any that keep to these rules, and one draw needn't show every extreme that they name: `expert_ids`: A token's 2 experts differ. Among the 128 tokens of one index of ep (aligned blocks of rows) no expert is named more than 48 times, and in some block one expert is named exactly 48 times.
All inputs are finite; a program needn't handle non-finite values.
Results may differ from the reference program's by a relative error of at most 0.014.
Values may be sent and summed in bfloat16 or wider, within the bound.
A program may use at most 128 MiB of HBM per device.

```python
import math
import jax
import jax.numpy as jnp
import numpy as np
from jax import lax

D = 2048
HEADS = 32
DK = 64
FF = 1024
N_GROUPS = 4
TOPK = 2
SEQ_GRP = 128
TOKENS = 512
EXPERTS = 8
EXP_GROUP = 2
CAP = 48
N_EP = 4


def steps_of(rng, shape, split, low, largest):
    loudness = 1.0
    for axis_at, shards_of in split:
        draws = jax.random.uniform(jax.random.fold_in(jax.random.fold_in(rng, 6), axis_at), (shards_of,), jnp.float32, low / len(split), largest / len(split))
        loudness = loudness * jnp.repeat(jnp.exp(draws), shape[axis_at] // shards_of).reshape((-1,) + (1,) * (len(shape) - 1 - axis_at))
    return loudness


def routed_block(own_key, own, number, rows, amount, top, most, slope):
    order = jax.random.permutation(own_key, amount)
    packed, usual = shares(amount, rows * top, most, slope, True), shares(amount, rows * top, most, slope, False)
    places = jnp.arange(amount)

    def named(tallies, turn):
        used = int((tallies > 0).sum())
        fixed = max(1, used // 4)
        shifted = fixed + (places - fixed + turn * (used - fixed)) % max(1, amount - fixed)
        return jnp.zeros((amount,), jnp.int32).at[order[jnp.where(places < fixed, places, shifted)]].set(jnp.asarray(tallies, jnp.int32))

    tallies = jnp.where(number % 4 == 0, named(packed, number // 4), named(usual, number - number // 4 - 1))
    mixed = jax.random.permutation(jax.random.fold_in(own, 3), amount)
    giver, receiver = mixed[0:amount // 2 * 2:2], mixed[1:amount // 2 * 2:2]
    slack = jnp.minimum(tallies[giver] - 1, most - tallies[receiver]) // 2
    slack = jnp.where((giver == order[0]) | (receiver == order[0]) | (tallies[receiver] == 0), 0, jnp.maximum(slack, 0))
    shifted = jax.random.randint(jax.random.fold_in(own, 4), (amount // 2,), 0, 1 << 20) % (slack + 1)
    tallies = tallies.at[giver].add(-shifted).at[receiver].add(shifted)
    labels = jnp.searchsorted(jnp.cumsum(tallies), jnp.arange(rows * top), side="right").astype(jnp.int32)
    grid = labels.reshape(top, rows).T
    grid = grid[jax.random.permutation(jax.random.fold_in(own, 1), rows)]
    turn = jax.random.randint(jax.random.fold_in(own, 2), (rows, 1), 0, top)
    return jnp.take_along_axis(grid, (jnp.arange(top)[None, :] + turn) % top, axis=1)


def shares(amount, total, bound, slope, full):
    loads = [(1 << 20) // math.isqrt(standing ** slope) + 1 for standing in range(1, amount + 1)]
    largest = bound if full else min(bound, max(-(-total // amount), total * loads[0] // sum(loads)))
    least = 1 if total - largest >= amount - 1 else 0
    holding, surplus = [largest] + [least] * (amount - 1), total - largest - least * (amount - 1)
    while surplus > 0:
        candidates = [i for i in range(1, amount) if holding[i] < largest] or [i for i in range(1, amount) if holding[i] < bound]
        whole, left = sum([loads[i] for i in candidates]), surplus
        for i in candidates:
            more = min(bound - holding[i], max(1, left * loads[i] // whole), surplus)
            holding[i] = holding[i] + more
            surplus = surplus - more
    return np.array(holding)


def normal_values(key, shape, spread, bound, cuts=(), kind=jnp.bfloat16):
    factor_of = steps_of(key, shape, cuts, -0.22, 0.18) if cuts else 1.0
    result = jax.random.normal(key, shape, jnp.float32) * spread * factor_of
    return jnp.minimum(jnp.maximum(result, -bound), bound).astype(kind)


def setup_inputs(seed: int = 0) -> dict:
    keys = jax.random.split(jax.random.key(seed), 22)
    resid = normal_values(keys[0], (TOKENS, D), 1.0, 6.0, ((0, 4),))
    norm1_gain = jnp.clip(1.0 + 0.18 * jax.random.normal(keys[1], (D,), jnp.float32), 0.1, 1.9)
    w_query = normal_values(keys[2], (D, HEADS * DK), D ** -0.5, 0.125, ((0, 4), (1, 8)))
    w_key = normal_values(keys[3], (D, HEADS * DK), D ** -0.5, 0.125, ((0, 4), (1, 8)))
    w_value = normal_values(keys[4], (D, HEADS * DK), D ** -0.5, 0.125, ((0, 4), (1, 8)))
    w_outgate = normal_values(keys[5], (D, HEADS * DK), D ** -0.5, 0.125, ((0, 4), (1, 8)))
    w_igate = normal_values(keys[6], (D, HEADS), D ** -0.5, 0.125)
    w_fgate = normal_values(keys[7], (D, HEADS), D ** -0.5, 0.125)
    forget_bias = jnp.clip(jax.random.uniform(keys[8], (HEADS,), jnp.float32, 0.0, 4.0), 0.0, 4.0)
    head_gain = jnp.clip(1.0 + 0.18 * jax.random.normal(keys[9], (HEADS * DK,), jnp.float32), 0.1, 1.9)
    w_out = normal_values(keys[10], (HEADS * DK, D), (HEADS * DK) ** -0.5, 0.125, ((0, 8),))
    state_matrix = normal_values(keys[11], (TOKENS, HEADS, DK, DK), 0.5, 4.0, ((0, 4), (1, 8)), jnp.float32)
    state_norm = normal_values(keys[12], (TOKENS, HEADS, DK), 2.0, 8.0, ((0, 4), (1, 8)), jnp.float32)
    state_max = jnp.clip(-1.0 + 3.0 * jax.random.uniform(keys[13], (TOKENS, HEADS), jnp.float32) ** steps_of(keys[13], (TOKENS, HEADS), ((0, 4), (1, 8)), -0.2, 0.2), -1.0, 2.0)
    norm2_gain = jnp.clip(1.0 + 0.18 * jax.random.normal(keys[14], (D,), jnp.float32), 0.1, 1.9)
    group_router = normal_values(keys[15], (D, N_GROUPS), D ** -0.5, 0.125)
    expert_router = normal_values(keys[16], (D, EXPERTS), D ** -0.5, 0.125)
    expert_ids_keys = jax.random.split(jax.random.fold_in(keys[17], 1), TOKENS // SEQ_GRP)
    expert_ids_turns = jax.random.permutation(jax.random.fold_in(keys[17], 3), TOKENS // SEQ_GRP)
    expert_ids = jax.vmap(lambda own, number: routed_block(jax.random.fold_in(keys[17], 2), own, number, SEQ_GRP, EXPERTS, TOPK, CAP, 2))(expert_ids_keys, expert_ids_turns).reshape((TOKENS, TOPK))
    exp_gate = normal_values(keys[18], (EXPERTS, D, FF), D ** -0.5, 0.125, ((0, 4), (2, 8)))
    exp_up = normal_values(keys[19], (EXPERTS, D, FF), D ** -0.5, 0.125, ((0, 4), (2, 8)))
    exp_down = normal_values(keys[20], (EXPERTS, FF, D), FF ** -0.5, 0.1875, ((0, 4), (1, 8)))
    return {"resid": resid, "norm1_gain": norm1_gain, "w_query": w_query, "w_key": w_key, "w_value": w_value, "w_outgate": w_outgate, "w_igate": w_igate, "w_fgate": w_fgate, "forget_bias": forget_bias, "head_gain": head_gain, "w_out": w_out, "state_matrix": state_matrix, "state_norm": state_norm, "state_max": state_max, "norm2_gain": norm2_gain, "group_router": group_router, "expert_router": expert_router, "expert_ids": expert_ids, "exp_gate": exp_gate, "exp_up": exp_up, "exp_down": exp_down}


EPSILON = 1e-06

def rms_scale(values, gain):
    widened = values.astype(jnp.float32)
    factor = lax.rsqrt(lax.optimization_barrier(jnp.mean(widened * widened, axis=-1, keepdims=True)) + EPSILON)
    return widened * factor * gain.astype(jnp.float32)

def memory_cell(scaled, key_rows, value_rows, in_gate, log_forget, matrix, normer, running):
    stable = jnp.maximum(log_forget + running, in_gate)
    fresh = jnp.exp(in_gate - stable)
    carried = jnp.exp(log_forget + running - stable)
    readout = jnp.einsum('bhd,bhde->bhe', scaled, matrix, precision=lax.Precision.HIGHEST)
    score = lax.optimization_barrier(jnp.sum(scaled * key_rows, axis=-1)) * fresh
    numer = carried[..., None] * readout + score[..., None] * value_rows
    denom = carried * lax.optimization_barrier(jnp.sum(scaled * normer, axis=-1)) + score
    cell_out = numer / jnp.maximum(jnp.abs(denom), 1.0)[..., None]
    new_matrix = carried[..., None, None] * matrix + fresh[..., None, None] * key_rows[..., :, None] * value_rows[..., None, :]
    new_normer = carried[..., None] * normer + fresh[..., None] * key_rows
    return (cell_out, new_matrix, new_normer, stable)

def reference(resid, norm1_gain, w_query, w_key, w_value, w_outgate, w_igate, w_fgate, forget_bias, head_gain, w_out, state_matrix, state_norm, state_max, norm2_gain, group_router, expert_router, expert_ids, exp_gate, exp_up, exp_down):
    rows = resid.shape[0]
    heads = state_matrix.shape[1]
    size = state_matrix.shape[2]
    normed = rms_scale(resid, norm1_gain).astype(jnp.bfloat16)

    def project(weight):
        product = jnp.dot(normed, weight, preferred_element_type=jnp.float32)
        stored = lax.optimization_barrier(product.astype(jnp.bfloat16))
        return stored.astype(jnp.float32).reshape(rows, heads, size)
    scaled = project(w_query) * size ** (-0.5)
    key_rows = project(w_key)
    value_rows = project(w_value)
    outgate = project(w_outgate)
    in_gate = jnp.dot(normed, w_igate, preferred_element_type=jnp.float32)
    log_forget = jax.nn.log_sigmoid(jnp.dot(normed, w_fgate, preferred_element_type=jnp.float32) + forget_bias)
    cell_out, new_matrix, new_normer, new_max = memory_cell(scaled, key_rows, value_rows, in_gate, log_forget, state_matrix, state_norm, state_max)
    headed = cell_out * lax.rsqrt(lax.optimization_barrier(jnp.mean(cell_out * cell_out, axis=-1, keepdims=True)) + EPSILON)
    headed = headed * head_gain.reshape(heads, size) * jax.nn.sigmoid(outgate)
    head_out = headed.astype(jnp.bfloat16).reshape(rows, heads * size)
    after_mix = (resid.astype(jnp.float32) + jnp.dot(head_out, w_out, preferred_element_type=jnp.float32)).astype(jnp.bfloat16)
    normed2 = rms_scale(after_mix, norm2_gain).astype(jnp.bfloat16)
    group_exp = jnp.exp(jnp.dot(normed2, group_router, preferred_element_type=jnp.float32))
    group_prob = group_exp / lax.optimization_barrier(jnp.sum(group_exp, axis=1, keepdims=True))
    expert_logits = jnp.dot(normed2, expert_router, preferred_element_type=jnp.float32)
    chosen_exp = jnp.exp(jnp.take_along_axis(expert_logits, expert_ids, axis=1))
    share = chosen_exp / lax.optimization_barrier(jnp.sum(chosen_exp, axis=1, keepdims=True))
    group_weight = jnp.take_along_axis(group_prob, expert_ids // EXP_GROUP, axis=1)
    route_weight = group_weight * share
    limit = CAP * N_EP

    def one_expert(total, inputs):
        expert_index, gate_w, up_w, down_w = inputs
        picked = expert_ids == expert_index
        coeff = lax.optimization_barrier(jnp.sum(jnp.where(picked, route_weight, 0.0), axis=1))
        member = jnp.any(picked, axis=1)
        count = jnp.sum(member.astype(jnp.int32))
        places = jnp.nonzero(member, size=limit, fill_value=0)[0].astype(jnp.int32)
        valid = (jnp.arange(limit, dtype=jnp.int32) < count).astype(jnp.float32)
        taken = normed2[places]
        gate_part = jnp.dot(taken, gate_w, preferred_element_type=jnp.float32)
        up_part = jnp.dot(taken, up_w, preferred_element_type=jnp.float32)
        units = (jax.nn.silu(gate_part) * up_part).astype(jnp.bfloat16)
        expert_out = jnp.dot(units, down_w, preferred_element_type=jnp.float32)
        total = total.at[places].add(expert_out * (coeff[places] * valid)[:, None])
        return (total, None)
    start_total = jnp.zeros((rows, resid.shape[1]), jnp.float32)
    moe, _ = lax.scan(one_expert, start_total, (jnp.arange(EXPERTS, dtype=jnp.int32), exp_gate, exp_up, exp_down))
    mixed = (after_mix.astype(jnp.float32) + moe).astype(jnp.bfloat16)
    return (mixed, new_matrix, new_normer, new_max)
```

```python
import functools

import jax
import jax.numpy as jnp
from jax import lax
from jax.experimental import pallas as pl
from jax.experimental.pallas import tpu as pltpu
from jax.sharding import PartitionSpec as P

EPSILON = 1e-06


def rms_scale(values, gain):
    widened = values.astype(jnp.float32)
    factor = lax.rsqrt(jnp.mean(widened * widened, axis=-1, keepdims=True) + EPSILON)
    return widened * factor * gain


def memory_cell(scaled, key_rows, value_rows, in_gate, log_forget, matrix, normer, running):
    stable = jnp.maximum(log_forget + running, in_gate)
    fresh = jnp.exp(in_gate - stable)
    carried = jnp.exp(log_forget + running - stable)
    readout = jnp.einsum("bhd,bhde->bhe", scaled, matrix, precision=lax.Precision.HIGHEST)
    score = jnp.sum(scaled * key_rows, axis=-1) * fresh
    numer = carried[..., None] * readout + score[..., None] * value_rows
    denom = carried * jnp.sum(scaled * normer, axis=-1) + score
    cell_out = numer / jnp.maximum(jnp.abs(denom), 1.0)[..., None]
    new_matrix = (
        carried[..., None, None] * matrix
        + fresh[..., None, None] * key_rows[..., :, None] * value_rows[..., None, :]
    )
    new_normer = carried[..., None] * normer + fresh[..., None] * key_rows
    return (cell_out, new_matrix, new_normer, stable)


MESH = pl.DeviceIdType.MESH
VMEM = pl.BlockSpec(memory_space=pltpu.VMEM)
ANY = pl.BlockSpec(memory_space=pl.ANY)


def remote(src, dst, send_sem, recv_sem, device):
    return pltpu.make_async_remote_copy(
        src_ref=src,
        dst_ref=dst,
        send_sem=send_sem,
        recv_sem=recv_sem,
        device_id=device,
        device_id_type=MESH,
    )


def greet(devices):
    barrier = pltpu.get_barrier_semaphore()
    for device in devices:
        pl.semaphore_signal(barrier, inc=1, device_id=device, device_id_type=MESH)


def project_kernel(
    n, resid, gain, wq, wk, wv, wo, wi, wf, out, in_gate, forget,
    blocks, arrived, sent, returned, weights, total, wsem, fs, fr, rs, rr,
):
    me = lax.axis_index("ep")
    ahead = [lax.rem(me + k, n) for k in range(n)]
    behind = [lax.rem(me + n - k, n) for k in range(n)]
    greet([{"ep": ahead[k]} for k in range(1, n)])
    width = wq.shape[1]
    depth = wq.shape[0]
    loads = []
    for i, w in enumerate((wq, wk, wv, wo)):
        load = pltpu.make_async_copy(w, weights.at[:, i * width : (i + 1) * width], wsem.at[i])
        load.start()
        loads.append(load)
    normed = rms_scale(resid[...], gain[...]).astype(jnp.bfloat16)
    for j in range(n):
        blocks[j] = normed[:, j * depth : (j + 1) * depth]
    pl.semaphore_wait(pltpu.get_barrier_semaphore(), n - 1)
    forward = {}
    for k in range(1, n):
        forward[k] = remote(blocks.at[ahead[k]], arrived.at[k], fs.at[k], fr.at[k], {"ep": ahead[k]})
        forward[k].start()
    in_gate[...] = jnp.dot(normed, wi[...], preferred_element_type=jnp.float32)
    forget[...] = jnp.dot(normed, wf[...], preferred_element_type=jnp.float32)
    for load in loads:
        load.wait()
    total[...] = jnp.dot(blocks[me], weights[...], preferred_element_type=jnp.float32)
    back = {}
    for k in range(1, n):
        forward[k].wait_recv()
        sent[k] = jnp.dot(arrived[k], weights[...], preferred_element_type=jnp.float32).astype(
            jnp.bfloat16
        )
        back[k] = remote(sent.at[k], returned.at[k], rs.at[k], rr.at[k], {"ep": behind[k]})
        back[k].start()
    for k in range(1, n):
        back[k].wait_recv()
        total[...] += returned[k].astype(jnp.float32)
    out[...] = total[...].astype(jnp.bfloat16)
    for k in range(1, n):
        forward[k].wait_send()
        back[k].wait_send()


def project(resid, gain, wq, wk, wv, wo, wi, wf):
    n = lax.axis_size("ep")
    rows = resid.shape[0]
    depth, width = wq.shape
    dma = pltpu.SemaphoreType.DMA
    bf16, f32 = jnp.bfloat16, jnp.float32
    return pl.pallas_call(
        functools.partial(project_kernel, n),
        out_shape=(
            jax.ShapeDtypeStruct((rows, 4 * width), bf16),
            jax.ShapeDtypeStruct((rows, wi.shape[1]), f32),
            jax.ShapeDtypeStruct((rows, wi.shape[1]), f32),
        ),
        in_specs=[VMEM, VMEM, ANY, ANY, ANY, ANY, VMEM, VMEM],
        out_specs=(VMEM, VMEM, VMEM),
        scratch_shapes=[
            pltpu.VMEM((n, rows, depth), bf16),
            pltpu.VMEM((n, rows, depth), bf16),
            pltpu.VMEM((n, rows, 4 * width), bf16),
            pltpu.VMEM((n, rows, 4 * width), bf16),
            pltpu.VMEM((depth, 4 * width), bf16),
            pltpu.VMEM((rows, 4 * width), f32),
            dma((4,)), dma((n,)), dma((n,)), dma((n,)), dma((n,)),
        ],
        compiler_params=pltpu.CompilerParams(
            collective_id=0, has_side_effects=True, vmem_limit_bytes=32 * 1024 * 1024
        ),
    )(resid, gain.reshape(1, -1), wq, wk, wv, wo, wi, wf)


def mix_kernel(
    nt, head, w, own_cols, after_out, full_out,
    full, pair_s, pair_r, red_s, red_r, gathered, ps, pr, rs, rr, gs, gr, os, orr,
):
    t = lax.axis_index("tp")
    nz = nt // 2
    z, c = t // 2, lax.rem(t, 2)
    partner = {"tp": t + 1 - 2 * c}
    ahead = [lax.rem(z + k, nz) for k in range(nz)]
    behind = [lax.rem(z + nz - k, nz) for k in range(nz)]
    peers = [{"tp": 2 * ahead[k] + c} for k in range(nz)]
    greet([partner] + peers[1:])
    cols = own_cols.shape[1]
    full[...] = jnp.dot(head[...], w[...], preferred_element_type=jnp.float32)

    def block(dest):
        return full[:, pl.ds(pl.multiple_of(dest * cols, cols), cols)]

    for k in range(nz):
        pair_s[k] = block(2 * ahead[k] + 1 - c).astype(jnp.bfloat16)
    pl.semaphore_wait(pltpu.get_barrier_semaphore(), nz)
    order = list(range(1, nz)) + [0]
    pair = {}
    for k in order:
        pair[k] = remote(pair_s.at[k], pair_r.at[k], ps.at[k], pr.at[k], partner)
        pair[k].start()
    reduce = {}
    for k in order:
        pair[k].wait_recv()
        value = block(2 * ahead[k] + c) + pair_r[k].astype(jnp.float32)
        if k == 0:
            total = value
        else:
            red_s[k] = value.astype(jnp.bfloat16)
            reduce[k] = remote(red_s.at[k], red_r.at[k], rs.at[k], rr.at[k], peers[k])
            reduce[k].start()
    for k in range(1, nz):
        reduce[k].wait_recv()
        total = total + red_r[k].astype(jnp.float32)
    after = (own_cols[...].astype(jnp.float32) + total).astype(jnp.bfloat16)
    after_out[...] = after
    gathered[t] = after
    gather, over = {}, {}
    for k in range(1, nz):
        gather[k] = remote(gathered.at[t], gathered.at[t], gs.at[k], gr.at[k], peers[k])
        gather[k].start()
    for k in range(nz):
        origin = 2 * behind[k] + c
        if k > 0:
            gather[k].wait_recv()
        over[k] = remote(gathered.at[origin], gathered.at[origin], os.at[k], orr.at[k], partner)
        over[k].start()
    for k in range(nz):
        over[k].wait_recv()
    for j in range(nt):
        full_out[:, j * cols : (j + 1) * cols] = gathered[j]
    for k in range(nz):
        pair[k].wait_send()
        over[k].wait_send()
        if k > 0:
            reduce[k].wait_send()
            gather[k].wait_send()


def mix(head, w, own_cols):
    nt = lax.axis_size("tp")
    nz = nt // 2
    rows, cols = own_cols.shape
    dma = pltpu.SemaphoreType.DMA
    bf16, f32 = jnp.bfloat16, jnp.float32
    return pl.pallas_call(
        functools.partial(mix_kernel, nt),
        out_shape=(
            jax.ShapeDtypeStruct((rows, cols), bf16),
            jax.ShapeDtypeStruct((rows, cols * nt), bf16),
        ),
        in_specs=[VMEM, VMEM, VMEM],
        out_specs=(VMEM, VMEM),
        scratch_shapes=[
            pltpu.VMEM((rows, cols * nt), f32),
            pltpu.VMEM((nz, rows, cols), bf16),
            pltpu.VMEM((nz, rows, cols), bf16),
            pltpu.VMEM((nz, rows, cols), bf16),
            pltpu.VMEM((nz, rows, cols), bf16),
            pltpu.VMEM((nt, rows, cols), bf16),
        ]
        + [dma((nz,))] * 8,
        compiler_params=pltpu.CompilerParams(
            collective_id=1, has_side_effects=True, vmem_limit_bytes=32 * 1024 * 1024
        ),
    )(head, w, own_cols)


def expert_kernel(
    n, nt, disp, comb, wg, wu, wd, out,
    arr, vg, vu, vd, full, pair_s, pair_r, ret_s, ret_r, z_s, z_r,
    wsem, ds, dr, fs, fr, ps, pr, rs, rr, zs, zr,
):
    me = lax.axis_index("ep")
    t = lax.axis_index("tp")
    nz = nt // 2
    z, c = t // 2, lax.rem(t, 2)
    partner = {"tp": t + 1 - 2 * c}
    ahead = [lax.rem(me + k, n) for k in range(n)]
    behind = [lax.rem(me + n - k, n) for k in range(n)]
    z_ahead = [lax.rem(z + k, nz) for k in range(nz)]
    z_peers = [{"tp": 2 * z_ahead[k] + c} for k in range(nz)]
    greet([{"ep": ahead[k]} for k in range(1, n)] + [partner] + z_peers[1:])
    loads = []
    for i, (w, v) in enumerate(((wg, vg), (wu, vu), (wd, vd))):
        load = pltpu.make_async_copy(w, v, wsem.at[i])
        load.start()
        loads.append(load)
    half = arr.shape[3]
    local = vg.shape[0]
    cap = disp.shape[1] // local
    cols = out.shape[1]
    pl.semaphore_wait(pltpu.get_barrier_semaphore(), n - 1 + nz)
    mine = pl.ds(pl.multiple_of(c * half, half), half)
    send, pass_on, pair, ret = {}, {}, {}, {}
    for k in range(1, n):
        send[k] = remote(
            disp.at[ahead[k], :, mine], arr.at[c, k], ds.at[k], dr.at[k], {"ep": ahead[k]}
        )
        send[k].start()
    arr[0, 0] = disp[me, :, :half]
    arr[1, 0] = disp[me, :, half:]
    for load in loads:
        load.wait()

    def block(k, dest):
        return full[k, :, pl.ds(pl.multiple_of(dest * cols, cols), cols)]

    def compute(k):
        for e in range(local):
            lines = slice(e * cap, (e + 1) * cap)
            low, high = arr[0, k, lines, :], arr[1, k, lines, :]

            def both(v):
                return jnp.dot(
                    low, v[e, :half, :], preferred_element_type=jnp.float32
                ) + jnp.dot(high, v[e, half:, :], preferred_element_type=jnp.float32)

            units = (jax.nn.silu(both(vg)) * both(vu)).astype(jnp.bfloat16)
            full[k, lines, :] = jnp.dot(units, vd[e], preferred_element_type=jnp.float32)
        for i in range(nz):
            pair_s[k, i] = block(k, 2 * i + 1 - c).astype(jnp.bfloat16)
        pair[k] = remote(pair_s.at[k], pair_r.at[k], ps.at[k], pr.at[k], partner)
        pair[k].start()

    def reply(k):
        pair[k].wait_recv()
        for i in range(nz):
            ret_s[k, i] = (block(k, 2 * i + c) + pair_r[k, i].astype(jnp.float32)).astype(
                jnp.bfloat16
            )
        if k > 0:
            ret[k] = remote(ret_s.at[k], ret_r.at[k], rs.at[k], rr.at[k], {"ep": behind[k]})
            ret[k].start()

    compute(0)
    for k in range(1, n):
        send[k].wait_recv()
        pass_on[k] = remote(arr.at[c, k], arr.at[c, k], fs.at[k], fr.at[k], partner)
        pass_on[k].start()
        pass_on[k].wait_recv()
        compute(k)
        reply(k)
    reply(0)
    ret_r[0] = ret_s[0]
    weights = []
    for k in range(n):
        exact = comb[ahead[k]]
        coarse = exact.astype(jnp.bfloat16)
        weights.append((coarse, (exact - coarse.astype(jnp.float32)).astype(jnp.bfloat16)))
        if k > 0:
            ret[k].wait_recv()
    gather = {}
    for i in list(range(1, nz)) + [0]:
        total = jnp.zeros(out.shape, jnp.float32)
        for k in range(n):
            part = ret_r[k, z_ahead[i]]
            for weight in weights[k]:
                total = total + jnp.dot(weight, part, preferred_element_type=jnp.float32)
        if i > 0:
            z_s[i] = total.astype(jnp.bfloat16)
            gather[i] = remote(z_s.at[i], z_r.at[i], zs.at[i], zr.at[i], z_peers[i])
            gather[i].start()
    for i in range(1, nz):
        gather[i].wait_recv()
        total = total + z_r[i].astype(jnp.float32)
    out[...] = total
    for k in range(n):
        pair[k].wait_send()
        if k > 0:
            send[k].wait_send()
            pass_on[k].wait_send()
            ret[k].wait_send()
    for i in range(1, nz):
        gather[i].wait_send()


def experts(disp, comb, wg, wu, wd):
    n, nt = lax.axis_size("ep"), lax.axis_size("tp")
    nz = nt // 2
    slots, width = disp.shape[1:]
    rows = comb.shape[1]
    cols = width // nt
    dma = pltpu.SemaphoreType.DMA
    bf16, f32 = jnp.bfloat16, jnp.float32
    return pl.pallas_call(
        functools.partial(expert_kernel, n, nt),
        out_shape=jax.ShapeDtypeStruct((rows, cols), f32),
        in_specs=[VMEM, VMEM, ANY, ANY, ANY],
        out_specs=VMEM,
        scratch_shapes=[
            pltpu.VMEM((2, n, slots, width // 2), bf16),
            pltpu.VMEM(wg.shape, bf16),
            pltpu.VMEM(wu.shape, bf16),
            pltpu.VMEM(wd.shape, bf16),
            pltpu.VMEM((n, slots, width), f32),
            pltpu.VMEM((n, nz, slots, cols), bf16),
            pltpu.VMEM((n, nz, slots, cols), bf16),
            pltpu.VMEM((n, nz, slots, cols), bf16),
            pltpu.VMEM((n, nz, slots, cols), bf16),
            pltpu.VMEM((nz, rows, cols), bf16),
            pltpu.VMEM((nz, rows, cols), bf16),
            dma((3,)),
        ]
        + [dma((n,))] * 8
        + [dma((nz,))] * 2,
        compiler_params=pltpu.CompilerParams(
            collective_id=2, has_side_effects=True, vmem_limit_bytes=48 * 1024 * 1024
        ),
    )(disp, comb, wg, wu, wd)


def per_device(
    resid,
    norm1_gain,
    w_query,
    w_key,
    w_value,
    w_outgate,
    w_igate,
    w_fgate,
    forget_bias,
    head_gain,
    w_out,
    state_matrix,
    state_norm,
    state_max,
    norm2_gain,
    group_router,
    expert_router,
    expert_ids,
    exp_gate,
    exp_up,
    exp_down,
):
    rows = resid.shape[0]
    local_heads = state_matrix.shape[1]
    size = state_matrix.shape[2]
    head_rank = lax.axis_index("tp")
    projected, in_all, forget_all = project(
        resid, norm1_gain, w_query, w_key, w_value, w_outgate, w_igate, w_fgate
    )
    stored = projected.astype(jnp.float32)
    pieces = jnp.split(stored, 4, axis=1)
    scaled = pieces[0].reshape(rows, local_heads, size) * size ** (-0.5)
    key_rows = pieces[1].reshape(rows, local_heads, size)
    value_rows = pieces[2].reshape(rows, local_heads, size)
    outgate = pieces[3].reshape(rows, local_heads, size)
    head_start = head_rank * local_heads
    bias_slice = lax.dynamic_slice_in_dim(forget_bias, head_start, local_heads, 0)
    in_gate = lax.dynamic_slice_in_dim(in_all, head_start, local_heads, 1)
    log_forget = jax.nn.log_sigmoid(
        lax.dynamic_slice_in_dim(forget_all, head_start, local_heads, 1) + bias_slice
    )
    cell_out, new_matrix, new_normer, new_max = memory_cell(
        scaled, key_rows, value_rows, in_gate, log_forget, state_matrix, state_norm, state_max
    )
    headed = cell_out * lax.rsqrt(jnp.mean(cell_out * cell_out, axis=-1, keepdims=True) + EPSILON)
    headed = headed * head_gain.reshape(local_heads, size) * jax.nn.sigmoid(outgate)
    head_out = headed.astype(jnp.bfloat16).reshape(rows, local_heads * size)
    column_count = resid.shape[1] // lax.axis_size("tp")
    own_cols = lax.dynamic_slice_in_dim(resid, head_rank * column_count, column_count, 1)
    after_cols, after_mix = mix(head_out, w_out, own_cols)
    normed2 = rms_scale(after_mix, norm2_gain).astype(jnp.bfloat16)
    experts_all = expert_router.shape[1]
    groups = group_router.shape[1]
    per_group = experts_all // groups
    topk = expert_ids.shape[1]
    group_exp = jnp.exp(jnp.dot(normed2, group_router, preferred_element_type=jnp.float32))
    group_prob = group_exp / jnp.sum(group_exp, axis=1, keepdims=True)
    expert_logits = jnp.dot(normed2, expert_router, preferred_element_type=jnp.float32)
    expert_range = jnp.arange(experts_all, dtype=jnp.int32)
    one_hot = (expert_ids[:, :, None] == expert_range).astype(jnp.float32)
    chosen_exp = jnp.exp(jnp.sum(one_hot * expert_logits[:, None, :], axis=2))
    share = chosen_exp / jnp.sum(chosen_exp, axis=1, keepdims=True)
    group_hot = (
        (expert_ids // per_group)[:, :, None] == jnp.arange(groups, dtype=jnp.int32)
    ).astype(jnp.float32)
    group_weight = jnp.sum(group_hot * group_prob[:, None, :], axis=2)
    route_weight = group_weight * share
    capacity = max(2, 3 * rows * topk // (2 * experts_all))
    capacity = -(-capacity // 16) * 16
    flat_hot = one_hot.reshape(rows * topk, experts_all)
    earlier = jnp.cumsum(flat_hot, axis=0) - flat_hot
    slot = jnp.sum(earlier * flat_hot, axis=1).astype(jnp.int32).reshape(rows, topk)
    position = expert_ids * capacity + slot
    slot_range = jnp.arange(experts_all * capacity, dtype=jnp.int32)
    matched = position[:, :, None] == slot_range
    dispatch = jnp.any(matched, axis=1).astype(jnp.bfloat16)
    ep_count = lax.axis_size("ep")
    spread = matched.astype(jnp.float32) * route_weight[:, :, None]
    combine = jnp.sum(spread, axis=1).reshape(rows, ep_count, -1).transpose(1, 0, 2)
    buffer = jnp.einsum("ts,td->sd", dispatch, normed2, preferred_element_type=jnp.float32).astype(
        jnp.bfloat16
    )
    buffer = buffer.reshape(ep_count, -1, normed2.shape[1])
    moe = experts(buffer, combine, exp_gate, exp_up, exp_down)
    mixed = (after_cols.astype(jnp.float32) + moe).astype(jnp.bfloat16)
    return (mixed, new_matrix, new_normer, new_max)


def solution(mesh):
    in_specs = (
        P("ep", None),
        P(),
        P("ep", "tp"),
        P("ep", "tp"),
        P("ep", "tp"),
        P("ep", "tp"),
        P(),
        P(),
        P(),
        P("tp"),
        P("tp", None),
        P("ep", "tp", None, None),
        P("ep", "tp", None),
        P("ep", "tp"),
        P(),
        P(),
        P(),
        P("ep", None),
        P("ep", None, "tp"),
        P("ep", None, "tp"),
        P("ep", "tp", None),
    )
    out_specs = (P("ep", "tp"), P("ep", "tp", None, None), P("ep", "tp", None), P("ep", "tp"))
    return jax.shard_map(
        per_device, mesh=mesh, in_specs=in_specs, out_specs=out_specs, check_vma=False
    )
```
